32 devices in a mesh: ep: 8 (over z, y), tp: 4 (over x, core).
Axes of the slice: x: 2, y: 2, z: 4, core: 2. Of those that a mesh axis runs over, the one named last changes fastest.
Arguments:
- pool_input: bfloat16 [4096, 2048], P(('ep', 'tp')), may hold values from -6 to 6
- pool_gain: bfloat16 [2048], replicated, may hold values from 0.099609375 to 1.8984375
- pool_weight: bfloat16 [4, 512, 512], replicated, may hold values from -0.25 to 0.25
- pool_scale: bfloat16 [2048], replicated, may hold values from 0.099609375 to 1.8984375
- out_weight: bfloat16 [2048, 4096], P(None, 'tp'), may hold values from -0.125 to 0.125
- expert_input: bfloat16 [4096, 4096], P(('ep', 'tp')), may hold values from -6 to 6
- expert_gain: bfloat16 [4096], replicated, may hold values from 0.099609375 to 1.8984375
- route_ids: int32 [4096, 2], P('ep'), may hold values from 0 to 7, all different within a row; in each aligned block of 128 rows (0 to 127, 128 to 255, ...) at most 64 rows name the same one
- route_weights: float32 [4096, 2], P('ep'), may hold values from 0.1 to 1
- expert_gate: bfloat16 [8, 4096, 1024], P('ep', None, 'tp'), may hold values from -0.09375 to 0.09375
- expert_up: bfloat16 [8, 4096, 1024], P('ep', None, 'tp'), may hold values from -0.09375 to 0.09375
- expert_down: bfloat16 [8, 1024, 4096], P('ep', 'tp'), may hold values from -0.1875 to 0.1875
- shared_gate: bfloat16 [4096, 1024], P(None, 'tp'), may hold values from -0.09375 to 0.09375
- shared_up: bfloat16 [4096, 1024], P(None, 'tp'), may hold values from -0.09375 to 0.09375
- shared_down: bfloat16 [1024, 4096], P('tp'), may hold values from -0.1875 to 0.1875
Outputs:
- out_a: bfloat16 [4096, 4096], P('ep', 'tp')
- out_b: bfloat16 [4096, 4096], P(('ep', 'tp'))
The draws below stay inside these ranges and needn't reach their ends.
Inputs may be any that keep to these rules, and one draw needn't show every extreme that they name: `route_ids`: each row names 2 different experts. In each aligned block of 128 rows no expert is named by more than 64 rows, a bound that some block reaches.
All inputs are finite; a program needn't handle non-finite values.
Results may differ from the reference program's by a relative error of at most 0.012.
Values may be sent and summed in bfloat16 or wider, within the bound.
No kernel may reach another device: no remote copies, remote signals or barrier semaphores. Data moves between devices by JAX's collectives and lax.ppermute only.
A program may use at most 256 MiB of HBM per device.

```python
import math
from functools import partial
import jax
import jax.numpy as jnp
import numpy as np
from jax import lax

D = 4096
POOL_W = 2048
POOL_GW = 512
FF = 1024
SFF = 1024
TOP_K = 2
TOK_DEV = 128
TOKENS = 4096
EXPERTS = 8
CAP_DEV = 64
N_TP = 4


def level_of(rng, shape, cuts, least, top_value):
    loudness = 1.0
    for axis_at, blocks in cuts:
        steps = jax.random.uniform(jax.random.fold_in(jax.random.fold_in(rng, 6), axis_at), (blocks,), jnp.float32, least / len(cuts), top_value / len(cuts))
        loudness = loudness * jnp.repeat(jnp.exp(steps), shape[axis_at] // blocks).reshape((-1,) + (1,) * (len(shape) - 1 - axis_at))
    return loudness


def routed_block(key, own, number, rows, number_of, top, reach, skew):
    order = jax.random.permutation(key, number_of)
    packed, common = portions_of(number_of, rows * top, reach, skew, True), portions_of(number_of, rows * top, reach, skew, False)
    places = jnp.arange(number_of)

    def named(lengths, turn):
        used = int((lengths > 0).sum())
        fixed = max(1, used // 4)
        passed = fixed + (places - fixed + turn * (used - fixed)) % max(1, number_of - fixed)
        return jnp.zeros((number_of,), jnp.int32).at[order[jnp.where(places < fixed, places, passed)]].set(jnp.asarray(lengths, jnp.int32))

    lengths = jnp.where(number % 4 == 0, named(packed, number // 4), named(common, number - number // 4 - 1))
    mixed = jax.random.permutation(jax.random.fold_in(own, 3), number_of)
    donor, taker = mixed[0:number_of // 2 * 2:2], mixed[1:number_of // 2 * 2:2]
    slack = jnp.minimum(lengths[donor] - 1, reach - lengths[taker]) // 2
    slack = jnp.where((donor == order[0]) | (taker == order[0]) | (lengths[taker] == 0), 0, jnp.maximum(slack, 0))
    passed = jax.random.randint(jax.random.fold_in(own, 4), (number_of // 2,), 0, 1 << 20) % (slack + 1)
    lengths = lengths.at[donor].add(-passed).at[taker].add(passed)
    labels = jnp.searchsorted(jnp.cumsum(lengths), jnp.arange(rows * top), side="right").astype(jnp.int32)
    table = labels.reshape(top, rows).T
    table = table[jax.random.permutation(jax.random.fold_in(own, 1), rows)]
    turn = jax.random.randint(jax.random.fold_in(own, 2), (rows, 1), 0, top)
    return jnp.take_along_axis(table, (jnp.arange(top)[None, :] + turn) % top, axis=1)


def portions_of(count, total, most, slope, full):
    loads = [(1 << 20) // math.isqrt(grade ** slope) + 1 for grade in range(1, count + 1)]
    largest = most if full else min(most, max(-(-total // count), total * loads[0] // sum(loads)))
    least = 1 if total - largest >= count - 1 else 0
    given, surplus = [largest] + [least] * (count - 1), total - largest - least * (count - 1)
    while surplus > 0:
        free = [i for i in range(1, count) if given[i] < largest] or [i for i in range(1, count) if given[i] < most]
        pool, remaining = sum([loads[i] for i in free]), surplus
        for i in free:
            addition = min(most - given[i], max(1, remaining * loads[i] // pool), surplus)
            given[i] = given[i] + addition
            surplus = surplus - addition
    return np.array(given)


def normal_values(rng, shape, scale, most, cuts=(), held_as=jnp.bfloat16):
    entries = scale * jax.random.normal(rng, shape, jnp.float32)
    if cuts:
        entries = entries * level_of(rng, shape, cuts, -0.22, 0.18)
    return jnp.clip(entries, -most, most).astype(held_as)


def setup_inputs(seed: int = 0) -> dict:
    streams_of = jax.random.split(jax.random.key(seed), 16)
    pool_input = normal_values(streams_of[0], (TOKENS, POOL_W), 1.0, 6.0, ((0, 32),))
    pool_gain = jnp.clip(1.0 + 0.18 * jax.random.normal(streams_of[1], (POOL_W,), jnp.float32), 0.099609375, 1.8984375).astype(jnp.bfloat16)
    pool_weight = normal_values(streams_of[2], (4, POOL_GW, POOL_GW), POOL_GW ** -0.5, 0.25)
    pool_scale = jnp.clip(1.0 + 0.18 * jax.random.normal(streams_of[3], (POOL_W,), jnp.float32), 0.099609375, 1.8984375).astype(jnp.bfloat16)
    out_weight = normal_values(streams_of[4], (POOL_W, D), POOL_W ** -0.5, 0.125, ((1, 4),))
    expert_input = normal_values(streams_of[5], (TOKENS, D), 1.0, 6.0, ((0, 32),))
    expert_gain = jnp.clip(1.0 + 0.18 * jax.random.normal(streams_of[6], (D,), jnp.float32), 0.099609375, 1.8984375).astype(jnp.bfloat16)
    route_ids_keys = jax.random.split(jax.random.fold_in(streams_of[7], 1), TOKENS // TOK_DEV)
    route_ids_turns = jax.random.permutation(jax.random.fold_in(streams_of[7], 3), TOKENS // TOK_DEV)
    route_ids = jax.vmap(lambda own, number: routed_block(jax.random.fold_in(streams_of[7], 2), own, number, TOK_DEV, EXPERTS, TOP_K, CAP_DEV, 2))(route_ids_keys, route_ids_turns).reshape((TOKENS, TOP_K))
    route_weights = jnp.clip(0.1 + 0.9 * jax.random.uniform(streams_of[8], (TOKENS, TOP_K), jnp.float32) ** level_of(streams_of[8], (TOKENS, TOP_K), ((0, 8),), -0.2, 0.2), 0.1, 1.0)
    expert_gate = normal_values(streams_of[9], (EXPERTS, D, FF), D ** -0.5, 0.09375, ((0, 8), (2, 4)))
    expert_up = normal_values(streams_of[10], (EXPERTS, D, FF), D ** -0.5, 0.09375, ((0, 8), (2, 4)))
    expert_down = normal_values(streams_of[11], (EXPERTS, FF, D), FF ** -0.5, 0.1875, ((0, 8), (1, 4)))
    shared_gate = normal_values(streams_of[12], (D, SFF), D ** -0.5, 0.09375, ((1, 4),))
    shared_up = normal_values(streams_of[13], (D, SFF), D ** -0.5, 0.09375, ((1, 4),))
    shared_down = normal_values(streams_of[14], (SFF, D), SFF ** -0.5, 0.1875, ((0, 4),))
    return {"pool_input": pool_input, "pool_gain": pool_gain, "pool_weight": pool_weight, "pool_scale": pool_scale, "out_weight": out_weight, "expert_input": expert_input, "expert_gain": expert_gain, "route_ids": route_ids, "route_weights": route_weights, "expert_gate": expert_gate, "expert_up": expert_up, "expert_down": expert_down, "shared_gate": shared_gate, "shared_up": shared_up, "shared_down": shared_down}


epsilon = 1e-06
WINDOWS = (2, 4, 8, 16)
ROUTED_SCALE = 2.5
rim_rows = 15

def rms_scale(source, gain):
    values = source.astype(jnp.float32)
    inverse = lax.rsqrt(lax.optimization_barrier(jnp.mean(values * values, axis=-1, keepdims=True)) + epsilon)
    return (values * inverse * gain.astype(jnp.float32)).astype(jnp.bfloat16)

def pool_groups(padded, offset):
    length = padded.shape[0] - rim_rows
    channels = padded.shape[1] // len(WINDOWS)
    position = (offset + jnp.arange(length, dtype=jnp.int32)).astype(jnp.float32)[:, None] + 1.0
    pieces = []
    for group_index, span in enumerate(WINDOWS):
        columns = padded[:, group_index * channels:(group_index + 1) * channels]
        window_sum = jnp.zeros((length, channels), jnp.float32)
        for steps_back in range(span):
            window_sum = window_sum + columns[rim_rows - steps_back:rim_rows - steps_back + length]
        counted = jnp.minimum(position, float(span))
        pieces.append(window_sum / counted - columns[rim_rows:])
    return jnp.concatenate(pieces, axis=1).astype(jnp.bfloat16)

def mix_groups(pooled, pool_weight, pool_scale):
    count_rows = pooled.shape[0]
    grouped = pooled.reshape(count_rows, pool_weight.shape[0], pool_weight.shape[1]).astype(jnp.float32)
    mixed = jnp.einsum('rgc,gcd->rgd', grouped, pool_weight.astype(jnp.float32))
    return (mixed.reshape(count_rows, -1) * pool_scale.astype(jnp.float32)).astype(jnp.bfloat16)

def slot_numbers(expert_ids, experts):
    flattened = expert_ids.reshape(-1)
    onehot = (flattened[:, None] == jnp.arange(experts, dtype=jnp.int32)[None, :]).astype(jnp.int32)
    before = jnp.cumsum(onehot, axis=0) - onehot
    return lax.optimization_barrier(jnp.sum(before * onehot, axis=1)).reshape(expert_ids.shape)

def swiglu_parts(source, gate_w, up_w, down_w):
    gate_val = jnp.dot(source, gate_w, preferred_element_type=jnp.float32)
    up_val = jnp.dot(source, up_w, preferred_element_type=jnp.float32)
    activated = (jax.nn.silu(gate_val) * up_val).astype(jnp.bfloat16)
    span_units = activated.shape[1] // N_TP
    totals = jnp.zeros((source.shape[0], down_w.shape[1]), jnp.float32)
    for quarter in range(N_TP):
        partial_sum = jnp.dot(activated[:, quarter * span_units:(quarter + 1) * span_units], down_w[quarter * span_units:(quarter + 1) * span_units], preferred_element_type=jnp.float32).astype(jnp.bfloat16)
        totals = totals + partial_sum.astype(jnp.float32)
    return totals.astype(jnp.bfloat16)

def reference(pool_input, pool_gain, pool_weight, pool_scale, out_weight, expert_input, expert_gain, route_ids, route_weights, expert_gate, expert_up, expert_down, shared_gate, shared_up, shared_down):
    normed_a = rms_scale(pool_input, pool_gain)
    padded = jnp.concatenate([jnp.zeros((rim_rows, normed_a.shape[1]), jnp.float32), normed_a.astype(jnp.float32)], axis=0)
    pooled = pool_groups(padded, 0)
    mixed = mix_groups(pooled, pool_weight, pool_scale)
    out_a = jnp.dot(mixed, out_weight, preferred_element_type=jnp.float32).astype(jnp.bfloat16)
    normed_b = rms_scale(expert_input, expert_gain)
    total_rows = normed_b.shape[0]
    blocks = total_rows // TOK_DEV
    top_count = route_ids.shape[1]
    block_ids = route_ids.reshape(blocks, TOK_DEV, top_count)
    slots = jax.vmap(partial(slot_numbers, experts=EXPERTS))(block_ids)
    row_index = jnp.broadcast_to(jnp.arange(total_rows, dtype=jnp.int32).reshape(blocks, TOK_DEV, 1), block_ids.shape)
    block_index = jnp.broadcast_to(jnp.arange(blocks, dtype=jnp.int32).reshape(blocks, 1, 1), block_ids.shape)
    scaled = route_weights.astype(jnp.float32)
    scaled = scaled / lax.optimization_barrier(jnp.sum(scaled, axis=1, keepdims=True)) * ROUTED_SCALE
    slot_table = jnp.full((EXPERTS, blocks, CAP_DEV), total_rows, jnp.int32).at[block_ids, block_index, slots].set(row_index)
    slot_weight = jnp.zeros((EXPERTS, blocks, CAP_DEV), jnp.float32).at[block_ids, block_index, slots].set(scaled.reshape(blocks, TOK_DEV, top_count))
    padded_b = jnp.concatenate([normed_b, jnp.zeros((1, normed_b.shape[1]), jnp.bfloat16)], axis=0)

    def add_expert(summed, inputs):
        gate_w, up_w, down_w, table_rows, table_weight = inputs
        chosen = padded_b[table_rows.reshape(-1)]
        result = lax.optimization_barrier(swiglu_parts(chosen, gate_w, up_w, down_w)).astype(jnp.float32)
        return (summed.at[table_rows.reshape(-1)].add(result * table_weight.reshape(-1, 1)), None)
    summed, _ = lax.scan(add_expert, jnp.zeros((total_rows + 1, normed_b.shape[1]), jnp.float32), (expert_gate, expert_up, expert_down, slot_table, slot_weight))
    shared = lax.optimization_barrier(swiglu_parts(normed_b, shared_gate, shared_up, shared_down)).astype(jnp.float32)
    out_b = (shared + summed[:total_rows]).astype(jnp.bfloat16)
    return (out_a, out_b)
```

```python
import jax
import jax.numpy as jnp
from jax import lax
from jax.sharding import PartitionSpec as P

epsilon = 1e-06
WINDOWS = (2, 4, 8, 16)
ROUTED_SCALE = 2.5
rim_rows = 15


def passed_along(block, axis, distance):
    devices = range(lax.axis_size(axis))
    route = [(i - distance, i) for i in devices if i - distance in devices]
    return lax.ppermute(block, axis, route)


def rms_scale(source, gain):
    values = source.astype(jnp.float32)
    inverse = lax.rsqrt(jnp.mean(values * values, axis=-1, keepdims=True) + epsilon)
    return (values * inverse * gain.astype(jnp.float32)).astype(jnp.bfloat16)


def pool_groups(padded, offset):
    length = padded.shape[0] - rim_rows
    channels = padded.shape[1] // len(WINDOWS)
    position = (offset + jnp.arange(length, dtype=jnp.int32)).astype(jnp.float32)[:, None] + 1.0
    pieces = []
    for group_index, span in enumerate(WINDOWS):
        columns = padded[:, group_index * channels : (group_index + 1) * channels]
        window_sum = jnp.zeros((length, channels), jnp.float32)
        for steps_back in range(span):
            window_sum = (
                window_sum + columns[rim_rows - steps_back : rim_rows - steps_back + length]
            )
        counted = jnp.minimum(position, float(span))
        pieces.append(window_sum / counted - columns[rim_rows:])
    return jnp.concatenate(pieces, axis=1).astype(jnp.bfloat16)


def mix_groups(pooled, pool_weight, pool_scale):
    count_rows = pooled.shape[0]
    grouped = pooled.reshape(count_rows, pool_weight.shape[0], pool_weight.shape[1])
    mixed = jnp.einsum("rgc,gcd->rgd", grouped, pool_weight, preferred_element_type=jnp.float32)
    return (mixed.reshape(count_rows, -1) * pool_scale.astype(jnp.float32)).astype(jnp.bfloat16)


def swapped(block, step):
    devices = range(lax.axis_size("tp"))
    return lax.ppermute(block, "tp", [(i, i ^ step) for i in devices])


def halvings(size):
    steps = []
    while size > 1:
        size //= 2
        steps.append(size)
    return steps


def spread(block):
    pieces = {0: block}
    for step in halvings(lax.axis_size("tp")):
        pieces.update({m | step: swapped(piece, step) for m, piece in list(pieces.items())})
    return pieces


def gathered_in_order(block):
    pieces = spread(block)
    size = len(pieces)
    stacked = jnp.stack([pieces[m] for m in range(size)])
    own = lax.axis_index("tp")
    ordered = [lax.dynamic_index_in_dim(stacked, own ^ i, 0, keepdims=False) for i in range(size)]
    return jnp.concatenate(ordered, axis=0)


def scattered_sum(product):
    size = lax.axis_size("tp")
    sums = None
    for step in reversed(halvings(size)):
        keep = [m for m in range(0, size, 2 * step)]
        away = [m | step for m in keep]
        take = product if sums is None else (lambda rows, held=sums: [held[m] for m in rows])
        sent = [swapped(part.astype(jnp.bfloat16), step) for part in take(away)]
        kept = take(keep)
        sums = {
            m: part.astype(jnp.float32) + other.astype(jnp.float32)
            for m, part, other in zip(keep, kept, sent)
        }
    return sums[0]


def gated(source, gate_w, up_w):
    gate_val = jnp.dot(source, gate_w, preferred_element_type=jnp.float32)
    up_val = jnp.dot(source, up_w, preferred_element_type=jnp.float32)
    return (jax.nn.silu(gate_val) * up_val).astype(jnp.bfloat16)


def slot_masks(expert_ids, experts, capacity):
    rows = expert_ids.shape[0]
    named = expert_ids[:, :, None] == jnp.arange(experts, dtype=jnp.int32)
    chosen = jnp.any(named, axis=1)
    earlier = jnp.tril(jnp.ones((rows, rows), jnp.bfloat16), -1)
    before = jnp.dot(
        earlier, chosen.astype(jnp.bfloat16), preferred_element_type=jnp.float32
    ).astype(jnp.int32)
    slots = jnp.arange(capacity, dtype=jnp.int32)
    taken = chosen[:, :, None] & (before[:, :, None] == slots)
    return named, taken


def body(
    pool_input,
    pool_gain,
    pool_weight,
    pool_scale,
    out_weight,
    expert_input,
    expert_gain,
    route_ids,
    route_weights,
    expert_gate,
    expert_up,
    expert_down,
    shared_gate,
    shared_up,
    shared_down,
):
    tok_rows = pool_input.shape[0]
    experts = lax.axis_size("ep")
    tp_index = lax.axis_index("tp")
    gates, ups, downs = spread(expert_gate[0]), spread(expert_up[0]), spread(expert_down[0])

    normed_b = rms_scale(expert_input, expert_gain)
    top_count = route_ids.shape[1]
    width_model = normed_b.shape[1]
    capacity = 2 * tok_rows * top_count // experts
    own_ids = lax.dynamic_slice_in_dim(route_ids, tp_index * tok_rows, tok_rows, 0)
    own_weights = lax.dynamic_slice_in_dim(route_weights, tp_index * tok_rows, tok_rows, 0)
    scaled = own_weights / jnp.sum(own_weights, axis=1, keepdims=True) * ROUTED_SCALE
    named, taken = slot_masks(own_ids, experts, capacity)
    place = taken.reshape(tok_rows, experts * capacity)
    outgoing = lax.dot_general(
        place.astype(jnp.bfloat16),
        normed_b,
        (((0,), (0,)), ((), ())),
        preferred_element_type=jnp.float32,
    ).astype(jnp.bfloat16)
    arrived = lax.all_to_all(
        outgoing.reshape(experts, capacity, width_model), "ep", split_axis=0, concat_axis=0, tiled=True
    ).reshape(-1, width_model)

    normed_a = rms_scale(pool_input, pool_gain)
    prev_rim = passed_along(normed_a[tok_rows - rim_rows :], ("ep", "tp"), 1)
    padded = jnp.concatenate([prev_rim, normed_a], axis=0).astype(jnp.float32)
    pooled = pool_groups(padded, lax.axis_index(("ep", "tp")) * tok_rows)
    mixed = mix_groups(pooled, pool_weight, pool_scale)
    out_a = jnp.dot(
        gathered_in_order(mixed), out_weight, preferred_element_type=jnp.float32
    ).astype(jnp.bfloat16)

    rows_b = spread(normed_b)

    def shared_product(members):
        rows = jnp.concatenate([rows_b[m] for m in members], axis=0)
        part = jnp.dot(
            gated(rows, shared_gate, shared_up), shared_down, preferred_element_type=jnp.float32
        ).astype(jnp.bfloat16)
        return [part[i * tok_rows : (i + 1) * tok_rows] for i in range(len(members))]

    shared_sum = scattered_sum(shared_product)

    totals = jnp.zeros((arrived.shape[0], width_model), jnp.float32)
    for m in gates:
        part = jnp.dot(
            gated(arrived, gates[m], ups[m]), downs[m], preferred_element_type=jnp.float32
        )
        totals = totals + part.astype(jnp.bfloat16).astype(jnp.float32)
    routed = totals.astype(jnp.bfloat16).reshape(experts, capacity, width_model)
    results = lax.all_to_all(routed, "ep", split_axis=0, concat_axis=0, tiled=True)
    results = results.reshape(experts * capacity, width_model)
    by_expert = jnp.sum(jnp.where(named, scaled[:, :, None], 0.0), axis=1)
    spread_scale = jnp.where(taken, by_expert[:, :, None], 0.0).reshape(tok_rows, -1)
    high = lax.reduce_precision(spread_scale, 8, 7)
    low = (spread_scale - high).astype(jnp.bfloat16)
    combined = jnp.dot(high.astype(jnp.bfloat16), results, preferred_element_type=jnp.float32)
    combined = combined + jnp.dot(low, results, preferred_element_type=jnp.float32)
    shared_out = shared_sum.astype(jnp.bfloat16).astype(jnp.float32)
    out_b = (shared_out + combined).astype(jnp.bfloat16)
    return (out_a, out_b)


def solution(mesh):
    in_specs = (
        P(("ep", "tp"), None),
        P(),
        P(),
        P(),
        P(None, "tp"),
        P(("ep", "tp"), None),
        P(),
        P("ep", None),
        P("ep", None),
        P("ep", None, "tp"),
        P("ep", None, "tp"),
        P("ep", "tp", None),
        P(None, "tp"),
        P(None, "tp"),
        P("tp", None),
    )
    out_specs = (P("ep", "tp"), P(("ep", "tp"), None))
    return jax.shard_map(body, mesh=mesh, in_specs=in_specs, out_specs=out_specs, check_vma=False)
```

```python
import jax
import jax.numpy as jnp
from jax import lax
from jax.sharding import PartitionSpec as P


epsilon = 1e-06
WINDOWS = (2, 4, 8, 16)
ROUTED_SCALE = 2.5
rim_rows = 15


def passed_along(block, axis, distance):
    devices = range(lax.axis_size(axis))
    route = [(i - distance, i) for i in devices if i - distance in devices]
    return lax.ppermute(block, axis, route)


def rms_scale(source, gain):
    values = source.astype(jnp.float32)
    inverse = lax.rsqrt(jnp.mean(values * values, axis=-1, keepdims=True) + epsilon)
    return (values * inverse * gain.astype(jnp.float32)).astype(jnp.bfloat16)


def pool_groups(padded, offset):
    length = padded.shape[0] - rim_rows
    channels = padded.shape[1] // len(WINDOWS)
    position = (offset + jnp.arange(length, dtype=jnp.int32)).astype(jnp.float32)[:, None] + 1.0
    pieces = []
    for group_index, span in enumerate(WINDOWS):
        columns = padded[:, group_index * channels : (group_index + 1) * channels]
        window_sum = jnp.zeros((length, channels), jnp.float32)
        for steps_back in range(span):
            window_sum = (
                window_sum + columns[rim_rows - steps_back : rim_rows - steps_back + length]
            )
        counted = jnp.minimum(position, float(span))
        pieces.append(window_sum / counted - columns[rim_rows:])
    return jnp.concatenate(pieces, axis=1).astype(jnp.bfloat16)


def mix_groups(pooled, pool_weight, pool_scale):
    count_rows = pooled.shape[0]
    grouped = pooled.reshape(count_rows, pool_weight.shape[0], pool_weight.shape[1])
    mixed = jnp.einsum("rgc,gcd->rgd", grouped, pool_weight, preferred_element_type=jnp.float32)
    return (mixed.reshape(count_rows, -1) * pool_scale.astype(jnp.float32)).astype(jnp.bfloat16)


def swapped(block, step):
    devices = range(lax.axis_size("tp"))
    return lax.ppermute(block, "tp", [(i, i ^ step) for i in devices])


def halvings(size):
    steps = []
    while size > 1:
        size //= 2
        steps.append(size)
    return steps


def spread(block):
    pieces = {0: block}
    for step in halvings(lax.axis_size("tp")):
        pieces.update({m | step: swapped(piece, step) for m, piece in list(pieces.items())})
    return pieces


def gathered_in_order(block):
    pieces = spread(block)
    size = len(pieces)
    stacked = jnp.stack([pieces[m] for m in range(size)])
    own = lax.axis_index("tp")
    ordered = [lax.dynamic_index_in_dim(stacked, own ^ i, 0, keepdims=False) for i in range(size)]
    return jnp.concatenate(ordered, axis=0)


def scattered_sum(product):
    size = lax.axis_size("tp")
    sums = None
    for step in reversed(halvings(size)):
        keep = [m for m in range(0, size, 2 * step)]
        away = [m | step for m in keep]
        take = product if sums is None else (lambda rows, held=sums: [held[m] for m in rows])
        sent = [swapped(part.astype(jnp.bfloat16), step) for part in take(away)]
        kept = take(keep)
        sums = {
            m: part.astype(jnp.float32) + other.astype(jnp.float32)
            for m, part, other in zip(keep, kept, sent)
        }
    return sums[0]


def gated(source, gate_w, up_w):
    gate_val = jnp.dot(source, gate_w, preferred_element_type=jnp.float32)
    up_val = jnp.dot(source, up_w, preferred_element_type=jnp.float32)
    return (jax.nn.silu(gate_val) * up_val).astype(jnp.bfloat16)


def slot_masks(expert_ids, experts, capacity):
    rows = expert_ids.shape[0]
    named = expert_ids[:, :, None] == jnp.arange(experts, dtype=jnp.int32)
    chosen = jnp.any(named, axis=1)
    earlier = jnp.tril(jnp.ones((rows, rows), jnp.bfloat16), -1)
    before = jnp.dot(
        earlier, chosen.astype(jnp.bfloat16), preferred_element_type=jnp.float32
    ).astype(jnp.int32)
    slots = jnp.arange(capacity, dtype=jnp.int32)
    taken = chosen[:, :, None] & (before[:, :, None] == slots)
    return named, taken


def body(
    pool_input,
    pool_gain,
    pool_weight,
    pool_scale,
    out_weight,
    expert_input,
    expert_gain,
    route_ids,
    route_weights,
    expert_gate,
    expert_up,
    expert_down,
    shared_gate,
    shared_up,
    shared_down,
):
    tok_rows = pool_input.shape[0]
    experts = lax.axis_size("ep")
    tp_index = lax.axis_index("tp")
    prev_rim = passed_along(pool_input[tok_rows - rim_rows :], ("ep", "tp"), 1)
    gates, ups = spread(expert_gate[0]), spread(expert_up[0])
    half = expert_down.shape[2] // 2
    downs = [spread(expert_down[0][:, :half]), spread(expert_down[0][:, half:])]

    normed_b = rms_scale(expert_input, expert_gain)
    top_count = route_ids.shape[1]
    width_model = normed_b.shape[1]
    capacity = 2 * tok_rows * top_count // experts
    own_ids = lax.dynamic_slice_in_dim(route_ids, tp_index * tok_rows, tok_rows, 0)
    own_weights = lax.dynamic_slice_in_dim(route_weights, tp_index * tok_rows, tok_rows, 0)
    scaled = own_weights / jnp.sum(own_weights, axis=1, keepdims=True) * ROUTED_SCALE
    named, taken = slot_masks(own_ids, experts, capacity)
    place = taken.reshape(tok_rows, experts * capacity)
    outgoing = lax.dot_general(
        place.astype(jnp.bfloat16),
        normed_b,
        (((0,), (0,)), ((), ())),
        preferred_element_type=jnp.float32,
    ).astype(jnp.bfloat16)
    outgoing = outgoing.reshape(experts, capacity, width_model)
    arrived = lax.all_to_all(outgoing, "ep", split_axis=0, concat_axis=0, tiled=True)
    arrived = arrived.reshape(-1, width_model)

    normed_a = rms_scale(pool_input, pool_gain)
    normed_rim = rms_scale(prev_rim, pool_gain)
    padded = jnp.concatenate([normed_rim, normed_a], axis=0).astype(jnp.float32)
    pooled = pool_groups(padded, lax.axis_index(("ep", "tp")) * tok_rows)
    mixed = mix_groups(pooled, pool_weight, pool_scale)
    out_a = jnp.dot(
        gathered_in_order(mixed), out_weight, preferred_element_type=jnp.float32
    ).astype(jnp.bfloat16)

    rows_b = spread(normed_b)

    def shared_product(members):
        rows = jnp.concatenate([rows_b[m] for m in members], axis=0)
        part = jnp.dot(
            gated(rows, shared_gate, shared_up), shared_down, preferred_element_type=jnp.float32
        ).astype(jnp.bfloat16)
        return [part[i * tok_rows : (i + 1) * tok_rows] for i in range(len(members))]

    shared_sum = scattered_sum(shared_product)

    order = list(gates)
    gate_whole = lax.optimization_barrier(jnp.concatenate([gates[m] for m in order], axis=1))
    up_whole = lax.optimization_barrier(jnp.concatenate([ups[m] for m in order], axis=1))
    activated = gated(arrived, gate_whole, up_whole)
    units = expert_down.shape[1]
    results = []
    for down in downs:
        totals = jnp.zeros((arrived.shape[0], half), jnp.float32)
        for place_of, m in enumerate(order):
            part = jnp.dot(
                activated[:, place_of * units : (place_of + 1) * units],
                down[m],
                preferred_element_type=jnp.float32,
            )
            totals = totals + part.astype(jnp.bfloat16).astype(jnp.float32)
        routed = totals.astype(jnp.bfloat16).reshape(experts, capacity, half)
        returned = lax.all_to_all(routed, "ep", split_axis=0, concat_axis=0, tiled=True)
        results.append(returned.reshape(experts * capacity, half))
    by_expert = jnp.sum(jnp.where(named, scaled[:, :, None], 0.0), axis=1)
    spread_scale = jnp.where(taken, by_expert[:, :, None], 0.0).reshape(tok_rows, -1)
    high = lax.reduce_precision(spread_scale, 8, 7)
    low = (spread_scale - high).astype(jnp.bfloat16)
    high = high.astype(jnp.bfloat16)
    combined = jnp.concatenate(
        [
            jnp.dot(high, rows, preferred_element_type=jnp.float32)
            + jnp.dot(low, rows, preferred_element_type=jnp.float32)
            for rows in results
        ],
        axis=1,
    )
    shared_out = shared_sum.astype(jnp.bfloat16).astype(jnp.float32)
    out_b = (shared_out + combined).astype(jnp.bfloat16)
    return (out_a, out_b)


def solution(mesh):
    in_specs = (
        P(("ep", "tp"), None),
        P(),
        P(),
        P(),
        P(None, "tp"),
        P(("ep", "tp"), None),
        P(),
        P("ep", None),
        P("ep", None),
        P("ep", None, "tp"),
        P("ep", None, "tp"),
        P("ep", "tp", None),
        P(None, "tp"),
        P(None, "tp"),
        P("tp", None),
    )
    out_specs = (P("ep", "tp"), P(("ep", "tp"), None))

    return jax.shard_map(body, mesh=mesh, in_specs=in_specs, out_specs=out_specs, check_vma=False)
```
